32 devices in a mesh: grp: 2 (over x), fs: 4 (over z), tp: 4 (over y, core).
Axes of the slice: x: 2, y: 2, z: 4, core: 2. Of those that a mesh axis runs over, the one named last changes fastest.
Arguments:
- tokens: bfloat16 [1024, 3584], P(('grp', 'fs')), parts along dimension 0, may hold values from -6 to 6
- norm_gain: float32 [3584], P('fs'), may hold values from 0.1 to 1.9
- up_master: float32 [3584, 14336], P('fs', 'tp'), may hold values from -0.09375 to 0.09375
- down_master: float32 [3584, 14336], P('fs', 'tp'), may hold values from -0.046875 to 0.046875
Outputs:
- up_ready: bfloat16 [7168, 14336], P('grp', 'tp'), parts along dimension 0
- down_ready: bfloat16 [7168, 14336], P('grp', 'tp'), parts along dimension 0
- mixed_out: bfloat16 [1024, 3584], P(('grp', 'fs', 'tp')), parts along dimension 0
The draws below stay inside these ranges and needn't reach their ends.
There are 2 independent parts, one for each index of `grp`. The reference program is written for one: setup_inputs(seed, part) draws one part's arguments, and reference() takes and returns one part's arrays. A program takes and returns all parts, laid end to end along the dimension named above; an argument that names none is the same for every part. Nothing has to cross between parts.
All inputs are finite; a program needn't handle non-finite values.
Results may differ from the reference program's by a relative error of at most 0.024.
Values may be sent and summed in bfloat16 or wider, within the bound.
A program may use at most 192 MiB of HBM per device.

```python
import jax
import jax.numpy as jnp
from jax import lax

D = 3584
FF = 14336
TOKENS = 512


def steps_of(own_key, shape, pieces, low, top_value):
    loudness = 1.0
    for position, blocks in pieces:
        draws = jax.random.uniform(jax.random.fold_in(jax.random.fold_in(own_key, 6), position), (blocks,), jnp.float32, low / len(pieces), top_value / len(pieces))
        loudness = loudness * jnp.repeat(jnp.exp(draws), shape[position] // blocks).reshape((-1,) + (1,) * (len(shape) - 1 - position))
    return loudness


def noise(rng, shape, scale, most, pieces=(), held_as=jnp.bfloat16):
    loudness = steps_of(rng, shape, pieces, -0.22, 0.18) if pieces else 1.0
    values = jax.random.normal(rng, shape, jnp.float32) * scale * loudness
    return jnp.minimum(jnp.maximum(values, -most), most).astype(held_as)


def setup_inputs(seed: int = 0, part: int = 0) -> dict:
    keys = jax.random.split(jax.random.key(seed), 5)
    part_splits = jax.random.split(jax.random.fold_in(keys[4], part), 5)
    tokens = noise(part_splits[0], (TOKENS, D), 1.0, 6.0, ((0, 4),))
    norm_gain = jnp.clip(1.0 + 0.18 * jax.random.normal(keys[1], (D,), jnp.float32), 0.1, 1.9)
    up_master = noise(keys[2], (D, FF), D ** -0.5, 0.09375, ((0, 4), (1, 4)), jnp.float32)
    down_master = noise(keys[3], (D, FF), FF ** -0.5, 0.046875, ((0, 4), (1, 4)), jnp.float32)
    return dict(tokens=tokens, norm_gain=norm_gain, up_master=up_master, down_master=down_master)


def reference(tokens, norm_gain, up_master, down_master):
    up_ready = (norm_gain[:, None] * up_master).astype(jnp.bfloat16)
    down_ready = down_master.astype(jnp.bfloat16)
    values = tokens.astype(jnp.float32)
    square_mean = lax.optimization_barrier(jnp.mean(values * values, axis=1, keepdims=True))
    normed = (values * lax.rsqrt(square_mean + 1e-06)).astype(jnp.bfloat16)
    up_acts = jnp.dot(normed, up_ready, preferred_element_type=jnp.float32)
    hidden = jnp.square(jax.nn.relu(up_acts)).astype(jnp.bfloat16)
    mixed_out = lax.dot_general(hidden, down_ready, (((1,), (1,)), ((), ())), preferred_element_type=jnp.float32)
    return (up_ready, down_ready, mixed_out.astype(jnp.bfloat16))
```

```python
import functools

import jax
import jax.numpy as jnp
from jax import lax
from jax.experimental import pallas as pl
from jax.experimental.pallas import tpu as pltpu
from jax.sharding import PartitionSpec as P

MESH = pl.DeviceIdType.MESH
VMEM_LIMIT = 60 * 1024 * 1024


def chunk_rows(half, width):
    for rows in range(16, half + 1, 16):
        if half % rows == 0 and rows * width * 2 >= 400 * 1024:
            return rows
    return half


def gather_kernel(sizes, gain, up, down, out, wide, narrow, load, store, zs, zr, own_s, xs, xr):
    groups, n, local, rows, count = sizes
    half = local // groups
    per = 2 * count
    g, f, t = lax.axis_index("grp"), lax.axis_index("fs"), lax.axis_index("tp")
    last = n - 1

    def loads(j, m):
        part = lax.rem(g + j, groups)
        master = (up, down)[m]

        def start(i, _):
            q = j * per + m * count + i
            first = pl.multiple_of(part * half + i * rows, 16)
            pltpu.make_async_copy(master.at[pl.ds(first, rows)], wide.at[q], load.at[q]).start()
            return _

        lax.fori_loop(0, count, start, 0)

    for j in range(groups):
        for m in range(2):
            loads(j, m)

    def where(source, part, q):
        m, i = q // count, q % count
        first = pl.multiple_of(source * local + part * half + i * rows, 16)
        return out.at[m, pl.ds(first, rows)]

    def convert(j, q):
        slot = j * per + q
        part = lax.rem(g + j, groups)
        pltpu.make_async_copy(up.at[pl.ds(0, rows)], wide.at[slot], load.at[slot]).wait()

        @pl.when(q < count)
        def _():
            first = pl.multiple_of(part * half + q * rows, 16)
            narrow[slot] = (gain[pl.ds(first, rows)] * wide[slot]).astype(jnp.bfloat16)

        @pl.when(q >= count)
        def _():
            narrow[slot] = wide[slot].astype(jnp.bfloat16)

    def keep(j, q):
        slot = j * per + q
        part = lax.rem(g + j, groups)
        return pltpu.make_async_copy(narrow.at[slot], where(f, part, q), store.at[slot])

    def own(way, q):
        to = f + 1 if way == 0 else f - 1
        return pltpu.make_async_remote_copy(
            narrow.at[q], where(f, g, q), own_s.at[way * per + q], zr.at[way * last * per + q],
            device_id=(g, to, t), device_id_type=MESH)

    def relay(way, k, q):
        source = f - k if way == 0 else f + k
        to = f + 1 if way == 0 else f - 1
        place = where(source, g, q)
        return pltpu.make_async_remote_copy(
            place, place, zs.at[(way * last + k - 1) * per + q], zr.at[(way * last + k) * per + q],
            device_id=(g, to, t), device_id_type=MESH)

    def arrival(way, k, q):
        source = f - k if way == 0 else f + k
        place = where(source, g, q)
        return pltpu.make_async_remote_copy(
            place, place, zs.at[0], zr.at[(way * last + k - 1) * per + q],
            device_id=(g, f, t), device_id_type=MESH)

    def across(j, way, k, q, part):
        source = f - k if way == 0 else f + k
        place = where(source, part, q)
        s = ((j * 2 + way) * last + k - 1) * per + q
        return pltpu.make_async_remote_copy(
            place, place, xs.at[s], xr.at[s],
            device_id=(lax.rem(g + 1 + j, groups), f, t), device_id_type=MESH)

    has = (f < last, f > 0)
    barrier = pltpu.get_barrier_semaphore()
    for way in range(2):
        @pl.when(has[way])
        def _(way=way):
            to = f + 1 if way == 0 else f - 1
            pl.semaphore_signal(barrier, inc=1, device_id=(g, to, t), device_id_type=MESH)
    for j in range(groups - 1):
        pl.semaphore_signal(barrier, inc=1, device_id=(lax.rem(g + 1 + j, groups), f, t), device_id_type=MESH)
    pl.semaphore_wait(barrier, groups - 1 + jnp.minimum(f, 1) + jnp.minimum(last - f, 1))

    def send_own(q):
        for way in range(2):
            @pl.when(has[way])
            def _(way=way):
                own(way, q).start()
        keep(0, q).start()

    def first_step(q, carry):
        convert(0, q)

        @pl.when(q > 0)
        def _():
            send_own(q - 1)
        return carry

    lax.fori_loop(0, per, first_step, 0)
    if groups > 1:
        convert(1, 0)
    send_own(per - 1)

    def step(k, q):
        for way in range(2):
            reach = (k <= f) if way == 0 else (k <= last - f)

            @pl.when(reach)
            def _(way=way):
                arrival(way, k, q).wait_recv()

                @pl.when(has[way])
                def _():
                    relay(way, k, q).start()
                for j in range(groups - 1):
                    across(j, way, k, q, g).start()

    def first_round(q, carry):
        step(1, q)
        for j in range(1, groups):
            if j > 1:
                convert(j, q)

            @pl.when(q + 1 < per)
            def _():
                if j == 1:
                    convert(1, q + 1)
            keep(j, q).start()
        return carry

    lax.fori_loop(0, per, first_round, 0)

    def later(r, carry):
        step(2 + r // per, r % per)
        return carry

    lax.fori_loop(0, (last - 1) * per, later, 0)

    def finish(r, carry):
        k, q = 1 + r // per, r % per
        for way in range(2):
            reach = (k <= f) if way == 0 else (k <= last - f)

            @pl.when(reach)
            def _(way=way):
                @pl.when(has[way])
                def _():
                    relay(way, k, q).wait_send()
                for j in range(groups - 1):
                    sender = lax.rem(g + groups - 1 - j, groups)
                    across(j, way, k, q, g).wait_send()
                    across(j, way, k, q, sender).wait_recv()
        return carry

    def finish_own(q, carry):
        for j in range(groups):
            keep(j, q).wait()
        for way in range(2):
            @pl.when(has[way])
            def _(way=way):
                own(way, q).wait_send()
        return carry

    lax.fori_loop(0, per, finish_own, 0)
    lax.fori_loop(0, last * per, finish, 0)


def gather(groups, n, gain, up, down):
    local, width = up.shape
    half = local // groups
    rows = chunk_rows(half, width)
    count = half // rows
    per = 2 * count
    last = n - 1
    dma = pltpu.SemaphoreType.DMA
    sent = 2 * (n - 1) * local * width * 2
    return pl.pallas_call(
        functools.partial(gather_kernel, (groups, n, local, rows, count)),
        out_shape=jax.ShapeDtypeStruct((2, n * local, width), jnp.bfloat16),
        in_specs=[pl.BlockSpec(memory_space=pltpu.VMEM)] + [pl.BlockSpec(memory_space=pl.ANY)] * 2,
        out_specs=pl.BlockSpec(memory_space=pl.ANY),
        scratch_shapes=[
            pltpu.VMEM((groups * per, rows, width), jnp.float32),
            pltpu.VMEM((groups * per, rows, width), jnp.bfloat16),
            dma((groups * per,)),
            dma((groups * per,)),
            dma((2 * last * per,)),
            dma((2 * last * per,)),
            dma((2 * per,)),
            dma((max(1, groups - 1) * 2 * last * per,)),
            dma((max(1, groups - 1) * 2 * last * per,)),
        ],
        compiler_params=pltpu.CompilerParams(
            collective_id=0, has_side_effects=True, vmem_limit_bytes=VMEM_LIMIT),
        cost_estimate=pl.CostEstimate(flops=0, bytes_accessed=sent, transcendentals=0),
        name="gather_both",
    )(gain[:, None], up, down)


def up_kernel(normed, block, ready, hidden, total):
    step = pl.program_id(0)

    @pl.when(step == 0)
    def _():
        total[...] = jnp.zeros_like(total)

    weights = block[0]
    ready[...] = weights
    total[...] += jnp.dot(normed[0], weights, preferred_element_type=jnp.float32)

    @pl.when(step == pl.num_programs(0) - 1)
    def _():
        hidden[...] = jnp.square(jnp.maximum(total[...], 0.0)).astype(jnp.bfloat16)


def down_kernel(hidden, block, ready, mixed):
    weights = block[0]
    ready[...] = weights
    mixed[0] = lax.dot_general(
        hidden[...], weights, (((1,), (1,)), ((), ())), preferred_element_type=jnp.float32
    ).astype(jnp.bfloat16)


def sum_kernel(tp, part, out, held, send, recv):
    g, f, t = lax.axis_index("grp"), lax.axis_index("fs"), lax.axis_index("tp")
    barrier = pltpu.get_barrier_semaphore()
    for j in range(1, tp):
        pl.semaphore_signal(barrier, inc=1, device_id=(g, f, lax.rem(t + j, tp)), device_id_type=MESH)
    pl.semaphore_wait(barrier, tp - 1)
    copies = []
    for j in range(1, tp):
        to = lax.rem(t + j, tp)
        copy = pltpu.make_async_remote_copy(
            part.at[to], held.at[j - 1], send.at[j - 1], recv.at[j - 1],
            device_id=(g, f, to), device_id_type=MESH)
        copy.start()
        copies.append(copy)
    total = part[t].astype(jnp.float32)
    for j in range(1, tp):
        copies[j - 1].wait()
        total = total + held[j - 1].astype(jnp.float32)
    out[...] = total.astype(jnp.bfloat16)


def per_device(groups, n, tp, tokens, norm_gain, up_master, down_master):
    values = tokens.astype(jnp.float32)
    square_mean = jnp.mean(values * values, axis=1, keepdims=True)
    normed = (values * lax.rsqrt(square_mean + 1e-06)).astype(jnp.bfloat16)
    both = gather(groups, n, norm_gain, up_master, down_master)
    depth, width = both.shape[1:]
    count = tokens.shape[0]
    steps = 8 if depth % (8 * 128) == 0 or depth % (8 * 16) == 0 else 1
    rows = depth // steps
    blocked = normed.reshape(count, steps, rows).transpose(1, 0, 2)
    ready_spec = pl.BlockSpec((rows, width), lambda i: (i, 0))
    weight = jax.ShapeDtypeStruct((depth, width), jnp.bfloat16)
    params = pltpu.CompilerParams(vmem_limit_bytes=VMEM_LIMIT)
    up_ready, hidden = pl.pallas_call(
        up_kernel,
        grid=(steps,),
        in_specs=[
            pl.BlockSpec((1, count, rows), lambda i: (i, 0, 0)),
            pl.BlockSpec((1, rows, width), lambda i: (0, i, 0)),
        ],
        out_specs=[ready_spec, pl.BlockSpec((count, width), lambda i: (0, 0))],
        out_shape=[weight, jax.ShapeDtypeStruct((count, width), jnp.bfloat16)],
        scratch_shapes=[pltpu.VMEM((count, width), jnp.float32)],
        compiler_params=params,
        name="up_pass",
    )(blocked, both)
    down_ready, mixed = pl.pallas_call(
        down_kernel,
        grid=(steps,),
        in_specs=[
            pl.BlockSpec((count, width), lambda i: (0, 0)),
            pl.BlockSpec((1, rows, width), lambda i: (1, i, 0)),
        ],
        out_specs=[ready_spec, pl.BlockSpec((1, count, rows), lambda i: (i, 0, 0))],
        out_shape=[weight, jax.ShapeDtypeStruct((steps, count, rows), jnp.bfloat16)],
        compiler_params=params,
        name="down_pass",
    )(hidden, both)
    share = count // tp
    parts = mixed.transpose(1, 0, 2).reshape(tp, share, depth)
    mixed_out = pl.pallas_call(
        functools.partial(sum_kernel, tp),
        out_shape=jax.ShapeDtypeStruct((share, depth), jnp.bfloat16),
        in_specs=[pl.BlockSpec(memory_space=pltpu.VMEM)],
        out_specs=pl.BlockSpec(memory_space=pltpu.VMEM),
        scratch_shapes=[
            pltpu.VMEM((tp - 1, share, depth), jnp.bfloat16),
            pltpu.SemaphoreType.DMA((tp - 1,)),
            pltpu.SemaphoreType.DMA((tp - 1,)),
        ],
        compiler_params=pltpu.CompilerParams(
            collective_id=1, has_side_effects=True, vmem_limit_bytes=VMEM_LIMIT),
        name="sum_shares",
    )(parts)
    return (up_ready, down_ready, mixed_out)


def solution(mesh):
    groups, n, tp = (mesh.shape[name] for name in ("grp", "fs", "tp"))
    return jax.shard_map(
        functools.partial(per_device, groups, n, tp),
        mesh=mesh,
        in_specs=(P(("grp", "fs"), None), P("fs"), P("fs", "tp"), P("fs", "tp")),
        out_specs=(P("grp", "tp"), P("grp", "tp"), P(("grp", "fs", "tp"), None)),
        check_vma=False,
    )
```

```python
import functools

import jax
import jax.numpy as jnp
from jax import lax
from jax.experimental import pallas as pl
from jax.experimental.pallas import tpu as pltpu
from jax.sharding import PartitionSpec as P

MESH = pl.DeviceIdType.MESH
VMEM_LIMIT = 60 * 1024 * 1024
ROWS = 512


def chunk_rows(half, width):
    for rows in range(16, half + 1, 16):
        if half % rows == 0 and rows * width * 2 >= 200 * 1024:
            return rows
    return half


def gather_kernel(sizes, gain, up, down, out, wide, narrow, load, store, zs, zr, own_s, xs, xr):
    groups, n, local, rows, count = sizes
    half = local // groups
    per = 2 * count
    g, f, t = lax.axis_index("grp"), lax.axis_index("fs"), lax.axis_index("tp")
    last = n - 1

    def loads(j, m):
        part = lax.rem(g + j, groups)
        master = (up, down)[m]

        def start(i, _):
            q = j * per + m * count + i
            first = pl.multiple_of(part * half + i * rows, 16)
            pltpu.make_async_copy(master.at[pl.ds(first, rows)], wide.at[q], load.at[q]).start()
            return _

        lax.fori_loop(0, count, start, 0)

    for j in range(groups):
        for m in range(2):
            loads(j, m)

    def where(source, part, q):
        m, i = q // count, q % count
        first = pl.multiple_of(source * local + part * half + i * rows, 16)
        return out.at[m, pl.ds(first, rows)]

    def convert(j, q):
        slot = j * per + q
        part = lax.rem(g + j, groups)
        pltpu.make_async_copy(up.at[pl.ds(0, rows)], wide.at[slot], load.at[slot]).wait()

        @pl.when(q < count)
        def _():
            first = pl.multiple_of(part * half + q * rows, 16)
            narrow[slot] = (gain[pl.ds(first, rows)] * wide[slot]).astype(jnp.bfloat16)

        @pl.when(q >= count)
        def _():
            narrow[slot] = wide[slot].astype(jnp.bfloat16)

    def keep(j, q):
        slot = j * per + q
        part = lax.rem(g + j, groups)
        return pltpu.make_async_copy(narrow.at[slot], where(f, part, q), store.at[slot])

    def own(way, q):
        to = f + 1 if way == 0 else f - 1
        return pltpu.make_async_remote_copy(
            narrow.at[q], where(f, g, q), own_s.at[way * per + q], zr.at[way * last * per + q],
            device_id=(g, to, t), device_id_type=MESH)

    def relay(way, k, q):
        source = f - k if way == 0 else f + k
        to = f + 1 if way == 0 else f - 1
        place = where(source, g, q)
        return pltpu.make_async_remote_copy(
            place, place, zs.at[(way * last + k - 1) * per + q], zr.at[(way * last + k) * per + q],
            device_id=(g, to, t), device_id_type=MESH)

    def arrival(way, k, q):
        source = f - k if way == 0 else f + k
        place = where(source, g, q)
        return pltpu.make_async_remote_copy(
            place, place, zs.at[0], zr.at[(way * last + k - 1) * per + q],
            device_id=(g, f, t), device_id_type=MESH)

    def across(j, way, k, q, part):
        source = f - k if way == 0 else f + k
        place = where(source, part, q)
        s = ((j * 2 + way) * last + k - 1) * per + q
        return pltpu.make_async_remote_copy(
            place, place, xs.at[s], xr.at[s],
            device_id=(lax.rem(g + 1 + j, groups), f, t), device_id_type=MESH)

    has = (f < last, f > 0)
    barrier = pltpu.get_barrier_semaphore()
    for way in range(2):
        @pl.when(has[way])
        def _(way=way):
            to = f + 1 if way == 0 else f - 1
            pl.semaphore_signal(barrier, inc=1, device_id=(g, to, t), device_id_type=MESH)
    for j in range(groups - 1):
        pl.semaphore_signal(barrier, inc=1, device_id=(lax.rem(g + 1 + j, groups), f, t), device_id_type=MESH)
    pl.semaphore_wait(barrier, groups - 1 + jnp.minimum(f, 1) + jnp.minimum(last - f, 1))

    def send_own(q):
        for way in range(2):
            @pl.when(has[way])
            def _(way=way):
                own(way, q).start()
        keep(0, q).start()

    def first_step(q, carry):
        convert(0, q)

        @pl.when(q > 0)
        def _():
            send_own(q - 1)
        return carry

    lax.fori_loop(0, per, first_step, 0)
    if groups > 1:
        convert(1, 0)
    send_own(per - 1)

    def step(k, q):
        for way in range(2):
            reach = (k <= f) if way == 0 else (k <= last - f)

            @pl.when(reach)
            def _(way=way):
                arrival(way, k, q).wait_recv()

                @pl.when(has[way])
                def _():
                    relay(way, k, q).start()
                for j in range(groups - 1):
                    across(j, way, k, q, g).start()

    def first_round(q, carry):
        step(1, q)
        for j in range(1, groups):
            if j > 1:
                convert(j, q)

            @pl.when(q + 1 < per)
            def _():
                if j == 1:
                    convert(1, q + 1)
            keep(j, q).start()
        return carry

    lax.fori_loop(0, per, first_round, 0)

    def later(r, carry):
        step(2 + r // per, r % per)
        return carry

    lax.fori_loop(0, (last - 1) * per, later, 0)

    def finish(r, carry):
        k, q = 1 + r // per, r % per
        for way in range(2):
            reach = (k <= f) if way == 0 else (k <= last - f)

            @pl.when(reach)
            def _(way=way):
                @pl.when(has[way])
                def _():
                    relay(way, k, q).wait_send()
                for j in range(groups - 1):
                    sender = lax.rem(g + groups - 1 - j, groups)
                    across(j, way, k, q, g).wait_send()
                    across(j, way, k, q, sender).wait_recv()
        return carry

    def finish_own(q, carry):
        for j in range(groups):
            keep(j, q).wait()
        for way in range(2):
            @pl.when(has[way])
            def _(way=way):
                own(way, q).wait_send()
        return carry

    lax.fori_loop(0, per, finish_own, 0)
    lax.fori_loop(0, last * per, finish, 0)


def gather(groups, n, gain, up, down):
    local, width = up.shape
    half = local // groups
    rows = chunk_rows(half, width)
    count = half // rows
    per = 2 * count
    last = n - 1
    dma = pltpu.SemaphoreType.DMA
    sent = 2 * (n - 1) * local * width * 2
    return pl.pallas_call(
        functools.partial(gather_kernel, (groups, n, local, rows, count)),
        out_shape=jax.ShapeDtypeStruct((2, n * local, width), jnp.bfloat16),
        in_specs=[pl.BlockSpec(memory_space=pltpu.VMEM)] + [pl.BlockSpec(memory_space=pl.ANY)] * 2,
        out_specs=pl.BlockSpec(memory_space=pl.ANY),
        scratch_shapes=[
            pltpu.VMEM((groups * per, rows, width), jnp.float32),
            pltpu.VMEM((groups * per, rows, width), jnp.bfloat16),
            dma((groups * per,)),
            dma((groups * per,)),
            dma((2 * last * per,)),
            dma((2 * last * per,)),
            dma((2 * per,)),
            dma((max(1, groups - 1) * 2 * last * per,)),
            dma((max(1, groups - 1) * 2 * last * per,)),
        ],
        compiler_params=pltpu.CompilerParams(
            collective_id=0, has_side_effects=True, vmem_limit_bytes=VMEM_LIMIT),
        cost_estimate=pl.CostEstimate(flops=0, bytes_accessed=sent, transcendentals=0),
        name="gather_both",
    )(gain[:, None], up, down)


def pass_kernel(steps, tokens, block, up_ready, down_ready, mixed, normed, total, hidden):
    step = pl.program_id(0)
    rows = block.shape[1]

    @pl.when(step == 0)
    def _():
        values = tokens[...].astype(jnp.float32)
        square_mean = jnp.mean(values * values, axis=1, keepdims=True)
        scaled = (values * lax.rsqrt(square_mean + 1e-06)).astype(jnp.bfloat16)
        for i in range(steps):
            normed[i] = scaled[:, i * rows:(i + 1) * rows]
        total[...] = jnp.zeros_like(total)

    @pl.when(step < steps)
    def _():
        weights = block[0]
        up_ready[...] = weights
        total[...] += jnp.dot(normed[step], weights, preferred_element_type=jnp.float32)

    @pl.when(step == steps - 1)
    def _():
        hidden[...] = jnp.square(jnp.maximum(total[...], 0.0)).astype(jnp.bfloat16)

    @pl.when(step >= steps)
    def _():
        weights = block[0]
        down_ready[...] = weights
        mixed[...] = lax.dot_general(
            hidden[...], weights, (((1,), (1,)), ((), ())), preferred_element_type=jnp.float32
        ).astype(jnp.bfloat16)


def sum_kernel(chips, part, out, pair, near, far, send, recv):
    g, f, t = lax.axis_index("grp"), lax.axis_index("fs"), lax.axis_index("tp")
    y, c = t // 2, lax.rem(t, 2)
    sibling = (g, f, 2 * y + 1 - c)

    def other(j):
        return lax.rem(y + j, chips)

    barrier = pltpu.get_barrier_semaphore()
    pl.semaphore_signal(barrier, inc=1, device_id=sibling, device_id_type=MESH)
    for j in range(1, chips):
        pl.semaphore_signal(barrier, inc=1, device_id=(g, f, 2 * other(j) + c), device_id_type=MESH)
    pl.semaphore_wait(barrier, chips)
    over, back = [], []
    for j in list(range(1, chips)) + [0]:
        copy = pltpu.make_async_remote_copy(
            part.at[2 * other(j) + 1 - c], near.at[j], send.at[j], recv.at[j],
            device_id=sibling, device_id_type=MESH)
        copy.start()
        over.append((j, copy))
    for j, copy in over:
        copy.wait_recv()
        both = part[2 * other(j) + c].astype(jnp.float32) + near[j].astype(jnp.float32)
        if j == 0:
            total = both
        else:
            pair[j] = both.astype(jnp.bfloat16)
            copy = pltpu.make_async_remote_copy(
                pair.at[j], far.at[j], send.at[chips + j], recv.at[chips + j],
                device_id=(g, f, 2 * other(j) + c), device_id_type=MESH)
            copy.start()
            back.append((j, copy))
    for j, copy in back:
        copy.wait_recv()
        total = total + far[j].astype(jnp.float32)
    out[...] = total.astype(jnp.bfloat16)
    for _, copy in over + back:
        copy.wait_send()


def per_device(groups, n, tp, tokens, norm_gain, up_master, down_master):
    both = gather(groups, n, norm_gain, up_master, down_master)
    depth, width = both.shape[1:]
    count = tokens.shape[0]
    rows = next(size for size in (ROWS, 256, 128, depth) if depth % size == 0)
    steps = depth // rows
    weight = jax.ShapeDtypeStruct((depth, width), jnp.bfloat16)
    up_ready, down_ready, mixed = pl.pallas_call(
        functools.partial(pass_kernel, steps),
        grid=(2 * steps,),
        in_specs=[
            pl.BlockSpec((count, depth), lambda i: (0, 0)),
            pl.BlockSpec((1, rows, width), lambda i: (i // steps, i % steps, 0)),
        ],
        out_specs=[
            pl.BlockSpec((rows, width), lambda i: (jnp.minimum(i, steps - 1), 0)),
            pl.BlockSpec((rows, width), lambda i: (jnp.maximum(i - steps, 0), 0)),
            pl.BlockSpec((count, rows), lambda i: (0, jnp.maximum(i - steps, 0))),
        ],
        out_shape=[weight, weight, jax.ShapeDtypeStruct((count, depth), jnp.bfloat16)],
        scratch_shapes=[
            pltpu.VMEM((steps, count, rows), jnp.bfloat16),
            pltpu.VMEM((count, width), jnp.float32),
            pltpu.VMEM((count, width), jnp.bfloat16),
        ],
        compiler_params=pltpu.CompilerParams(vmem_limit_bytes=VMEM_LIMIT),
        name="both_passes",
    )(tokens, both)
    share = count // tp
    chips = tp // 2
    held = pltpu.VMEM((chips, share, depth), jnp.bfloat16)
    mixed_out = pl.pallas_call(
        functools.partial(sum_kernel, chips),
        out_shape=jax.ShapeDtypeStruct((share, depth), jnp.bfloat16),
        in_specs=[pl.BlockSpec(memory_space=pltpu.VMEM)],
        out_specs=pl.BlockSpec(memory_space=pltpu.VMEM),
        scratch_shapes=[held, held, held] + [pltpu.SemaphoreType.DMA((2 * chips,))] * 2,
        compiler_params=pltpu.CompilerParams(
            collective_id=1, has_side_effects=True, vmem_limit_bytes=VMEM_LIMIT),
        name="sum_shares",
    )(mixed.reshape(tp, share, depth))
    return (up_ready, down_ready, mixed_out)


def solution(mesh):
    groups, n, tp = (mesh.shape[name] for name in ("grp", "fs", "tp"))
    return jax.shard_map(
        functools.partial(per_device, groups, n, tp),
        mesh=mesh,
        in_specs=(P(("grp", "fs"), None), P("fs"), P("fs", "tp"), P("fs", "tp")),
        out_specs=(P("grp", "tp"), P("grp", "tp"), P(("grp", "fs", "tp"), None)),
        check_vma=False,
    )
```
